32 devices in a mesh: grp: 2 (over y), kv: 4 (over z), tp: 4 (over x, core).
Axes of the slice: x: 2, y: 2, z: 4, core: 2. Of those that a mesh axis runs over, the one named last changes fastest.
Arguments:
- tokens: bfloat16 [16, 4, 2048], P('grp', None, 'kv'), parts along dimension 0, may hold values from -6 to 6
- prev_len: int32 [16], P('grp'), parts along dimension 0, may hold values from 1 to 1016, as said below
- accepted: int32 [16], P('grp'), parts along dimension 0, may hold values from 1 to 4, as said below
- parents: int32 [16, 4], P('grp'), parts along dimension 0, may hold values from -1 to 2, as said below
- cache_latent: bfloat16 [16, 1024, 256], P('grp', 'kv'), parts along dimension 0, may hold values from -210 to 210
- cache_rope: bfloat16 [16, 1024, 64], P('grp', 'kv'), parts along dimension 0, may hold values from -6 to 6
- g_pre: bfloat16 [2048], P('kv'), may hold values from 0.099609375 to 1.8984375
- w_down_q: bfloat16 [2048, 512], P('kv'), may hold values from -0.125 to 0.125
- w_down_kv: bfloat16 [2048, 256], P('kv'), may hold values from -0.125 to 0.125
- w_key_rope: bfloat16 [2048, 64], P('kv'), may hold values from -0.125 to 0.125
- g_q: bfloat16 [512], replicated, may hold values from 0.099609375 to 1.8984375
- w_up_q: bfloat16 [512, 16, 128], P(None, 'tp'), may hold values from -0.25 to 0.25
- w_q_rope: bfloat16 [512, 16, 64], P(None, 'tp'), may hold values from -0.25 to 0.25
- w_up_key: bfloat16 [256, 16, 128], P(None, 'tp'), may hold values from -0.375 to 0.375
- w_up_value: bfloat16 [256, 16, 128], P(None, 'tp'), may hold values from -0.375 to 0.375
- w_out: bfloat16 [2048, 2048], P('tp', 'kv'), may hold values from -0.125 to 0.125
- g_out: bfloat16 [2048], P('kv'), may hold values from 0.099609375 to 1.8984375
Outputs:
- mixed: bfloat16 [16, 4, 2048], P('grp', None, 'kv'), parts along dimension 0
- new_latent: bfloat16 [16, 1024, 256], P('grp', 'kv'), parts along dimension 0
- new_rope: bfloat16 [16, 1024, 64], P('grp', 'kv'), parts along dimension 0
The draws below stay inside these ranges and needn't reach their ends.
There are 2 independent parts, one for each index of `grp`. The reference program is written for one: setup_inputs(seed, part) draws one part's arguments, and reference() takes and returns one part's arrays. A program takes and returns all parts, laid end to end along the dimension named above; an argument that names none is the same for every part. Nothing has to cross between parts.
Inputs may be any that keep to these rules, and one draw needn't show every extreme that they name: `prev_len`: the largest length is reached by some sequence in every draw. `accepted`: the largest count is reached by some sequence in every draw. `parents`: each parent is -1 or an earlier proposal of the same sequence; the first proposal's parent is -1.
All inputs are finite; a program needn't handle non-finite values.
Results may differ from the reference program's by a relative error of at most 0.015.
The reference program's roundings to bfloat16 on the way (of `scaled`, `q_norm`, `q_nope`, `q_absorbed`, `q_rot`, `latent_new`, `key_new` and `head_out`) count: a program that leaves them out, or rounds other values in their place, can miss the bound.
Values may be sent and summed in bfloat16 or wider, within the bound.
A program may use at most 64 MiB of HBM per device.

```python
import math
import jax
import jax.numpy as jnp
from jax import lax

D = 2048
H = 16
HG = 4
QR = 512
KVR = 256
NOPE = 128
ROPE = 64
VD = 128
SEQS = 8
POS_DEV = 256
PROP = 4
LEN = 1024
N_KV = 4
N_TP = 4


def draw_prev_len(key, part):
    longest = LEN - 2 * PROP
    top_shift = max(int(math.log2(longest)), 1)
    key_one, key_two = jax.random.split(jax.random.fold_in(key, 3))
    raw_bits = jax.random.randint(key_one, (SEQS,), max(longest // 2, 1), longest)
    shifts = jax.random.randint(key_two, (SEQS,), 0, top_shift + 1)
    shorter = jnp.clip(jnp.right_shift(raw_bits, shifts), 1, longest - 1)
    seq_index = jnp.arange(SEQS, dtype=jnp.int32)
    return jnp.where(seq_index == part % SEQS, longest, shorter).astype(jnp.int32)


def draw_accepted(key, part):
    fewer = jax.random.randint(jax.random.fold_in(key, 11), (SEQS,), 1, PROP)
    seq_index = jnp.arange(SEQS, dtype=jnp.int32)
    return jnp.where(seq_index == part % SEQS, PROP, fewer).astype(jnp.int32)


def draw_parents(key, part):
    raw_bits = jax.random.randint(jax.random.fold_in(key, 5), (SEQS, PROP), 0, 1 << 20)
    slot_index = jnp.arange(PROP, dtype=jnp.int32)[None, :]
    return (raw_bits % (slot_index + 1) - 1).astype(jnp.int32)


def draw_cache_latent(key, part):
    key_one = jax.random.fold_in(jax.random.fold_in(key, 7), 0)
    values = jnp.clip(jax.random.normal(key_one, (SEQS, LEN, KVR), jnp.float32), -4.0, 4.0)
    return values.astype(jnp.bfloat16)


def levels(stream_key, dims, cuts, low, top_value):
    level, own = 1.0, jax.random.fold_in(stream_key, 6)
    for dim, blocks in cuts:
        draws = jnp.exp(jax.random.uniform(jax.random.fold_in(own, dim), (blocks,), jnp.float32, low / len(cuts), top_value / len(cuts)))
        level = level * jnp.repeat(draws, dims[dim] // blocks).reshape([-1 if axis == dim else 1 for axis in range(len(dims))])
    return level


def bell_draw(stream_key, extent, spread, reach, shards=(), kind=jnp.bfloat16):
    loudness = levels(stream_key, extent, shards, -0.22, 0.18) if shards else 1.0
    values = jax.random.normal(stream_key, extent, jnp.float32) * spread * loudness
    return jnp.minimum(jnp.maximum(values, -reach), reach).astype(kind)


def setup_inputs(seed: int = 0, part: int = 0) -> dict:
    arg_keys = jax.random.split(jax.random.key(seed), 18)
    own_keys = jax.random.split(jax.random.fold_in(arg_keys[17], part), 18)
    return {
        "tokens": bell_draw(own_keys[0], (SEQS, PROP, D), 1.0, 6.0, ((2, 4),)),
        "prev_len": draw_prev_len(jax.random.fold_in(jax.random.fold_in(arg_keys[17], part), 71), part),
        "accepted": draw_accepted(jax.random.fold_in(jax.random.fold_in(arg_keys[17], part), 71), part),
        "parents": draw_parents(jax.random.fold_in(jax.random.fold_in(arg_keys[17], part), 71), part),
        "cache_latent": draw_cache_latent(jax.random.fold_in(jax.random.fold_in(arg_keys[17], part), 71), part),
        "cache_rope": bell_draw(own_keys[5], (SEQS, LEN, ROPE), 1.0, 6.0, ((1, 4),)),
        "g_pre": jnp.clip(1.0 + 0.18 * jax.random.normal(arg_keys[6], (D,), jnp.float32), 0.099609375, 1.8984375).astype(jnp.bfloat16),
        "w_down_q": bell_draw(arg_keys[7], (D, QR), D ** -0.5, 0.125, ((0, 4),)),
        "w_down_kv": bell_draw(arg_keys[8], (D, KVR), D ** -0.5, 0.125, ((0, 4),)),
        "w_key_rope": bell_draw(arg_keys[9], (D, ROPE), D ** -0.5, 0.125, ((0, 4),)),
        "g_q": jnp.clip(1.0 + 0.18 * jax.random.normal(arg_keys[10], (QR,), jnp.float32), 0.099609375, 1.8984375).astype(jnp.bfloat16),
        "w_up_q": bell_draw(arg_keys[11], (QR, H, NOPE), QR ** -0.5, 0.25, ((1, 4),)),
        "w_q_rope": bell_draw(arg_keys[12], (QR, H, ROPE), QR ** -0.5, 0.25, ((1, 4),)),
        "w_up_key": bell_draw(arg_keys[13], (KVR, H, NOPE), KVR ** -0.5, 0.375, ((1, 4),)),
        "w_up_value": bell_draw(arg_keys[14], (KVR, H, VD), KVR ** -0.5, 0.375, ((1, 4),)),
        "w_out": bell_draw(arg_keys[15], (H * VD, D), (H * VD) ** -0.5, 0.125, ((0, 4), (1, 4))),
        "g_out": jnp.clip(1.0 + 0.18 * jax.random.normal(arg_keys[16], (D,), jnp.float32), 0.099609375, 1.8984375).astype(jnp.bfloat16),
    }


EPS = 1e-06
ROPE_BASE = 10000.0
NEG_INF = -1e+30

def normalize(vector, gain):
    return vector * lax.rsqrt(lax.optimization_barrier(jnp.mean(vector * vector, axis=-1, keepdims=True)) + EPS) * gain.astype(jnp.float32)

def plain_normalize(vector):
    return vector * lax.rsqrt(lax.optimization_barrier(jnp.mean(vector * vector, axis=-1, keepdims=True)) + EPS)

def rotate(vector, position):
    half_dim = vector.shape[-1] // 2
    frequency = ROPE_BASE ** (-jnp.arange(half_dim, dtype=jnp.float32) / half_dim)
    angles = position.astype(jnp.float32)[..., None] * frequency
    cosine = jnp.cos(angles)
    sine_part = jnp.sin(angles)
    front = vector[..., :half_dim]
    back_part = vector[..., half_dim:]
    return jnp.concatenate([front * cosine - back_part * sine_part, back_part * cosine + front * sine_part], axis=-1)

def ancestry(parents):
    seq_count, prop_count = parents.shape
    link = (parents[:, :, None] == jnp.arange(prop_count, dtype=jnp.int32)[None, None, :]).astype(jnp.float32)
    identity = jnp.eye(prop_count, dtype=jnp.float32)
    family = jnp.broadcast_to(identity, (seq_count, prop_count, prop_count))
    for repeat in range(prop_count):
        family = identity + jnp.einsum('sjk,skm->sjm', link, family)
    return family

def reference(tokens, prev_len, accepted, parents, cache_latent, cache_rope, g_pre, w_down_q, w_down_kv, w_key_rope, g_q, w_up_q, w_q_rope, w_up_key, w_up_value, w_out, g_out):
    f32 = jnp.float32
    bf16 = jnp.bfloat16
    seq_count, prop_count, model_dim = tokens.shape
    token_count = seq_count * prop_count
    head_count = w_up_q.shape[1]
    inv_root = (NOPE + ROPE) ** (-0.5)
    token_rows = tokens.reshape(token_count, model_dim).astype(f32)
    token_scale = lax.rsqrt(lax.optimization_barrier(jnp.sum(token_rows * token_rows, axis=1)) / model_dim + EPS)[:, None]
    scaled = (token_rows * g_pre.astype(f32)).astype(bf16)
    q_latent = jnp.dot(scaled, w_down_q, preferred_element_type=f32) * token_scale
    kv_latent = jnp.dot(scaled, w_down_kv, preferred_element_type=f32) * token_scale
    key_raw = jnp.dot(scaled, w_key_rope, preferred_element_type=f32) * token_scale
    valid_len = prev_len + accepted
    family = ancestry(parents)
    depths = (lax.optimization_barrier(jnp.sum(family, axis=2)) - 1.0).astype(jnp.int32)
    positions = (valid_len[:, None] + depths).reshape(token_count)
    q_norm = normalize(q_latent, g_q).astype(bf16)
    q_nope = jnp.dot(q_norm, w_up_q.reshape(QR, head_count * NOPE), preferred_element_type=f32).astype(bf16)
    q_nope = q_nope.reshape(token_count, head_count, NOPE)
    q_absorbed = jnp.einsum('thn,rhn->thr', q_nope.astype(f32), w_up_key.astype(f32)).astype(bf16)
    q_raw = jnp.dot(q_norm, w_q_rope.reshape(QR, head_count * ROPE), preferred_element_type=f32)
    q_rot = rotate(q_raw.reshape(token_count, head_count, ROPE), positions[:, None]).astype(bf16)
    latent_new = plain_normalize(kv_latent).astype(bf16)
    key_new = rotate(key_raw, positions).astype(bf16)
    query_lat = q_absorbed.reshape(seq_count, prop_count, head_count, KVR)
    query_rot = q_rot.reshape(seq_count, prop_count, head_count, ROPE)

    def one_sequence(items):
        lat_query, rot_query, latents, rot_keys, length = items
        scores = jnp.einsum('jhr,kr->jhk', lat_query.astype(f32), latents.astype(f32))
        scores = (scores + jnp.einsum('jhp,kp->jhk', rot_query.astype(f32), rot_keys.astype(f32))) * inv_root
        scores = scores.reshape(prop_count, head_count, N_KV, POS_DEV)
        visible = (jnp.arange(LEN, dtype=jnp.int32) < length).reshape(N_KV, POS_DEV)
        block_peak = lax.optimization_barrier(jnp.max(jnp.where(visible, scores, NEG_INF), axis=3))
        weights = jnp.where(visible, jnp.exp(scores - block_peak[..., None]), 0.0)
        block_mass = lax.optimization_barrier(jnp.sum(weights, axis=3))
        block_sum = jnp.einsum('jhbk,bkr->jhbr', weights.astype(bf16).astype(f32), latents.reshape(N_KV, POS_DEV, KVR).astype(f32))
        top_all = lax.optimization_barrier(jnp.max(block_peak, axis=2))
        factor = jnp.exp(block_peak - top_all[..., None])
        return (top_all, lax.optimization_barrier(jnp.sum(block_mass * factor, axis=2)), lax.optimization_barrier(jnp.sum(block_sum * factor[..., None], axis=2)))
    cache_peak, cache_mass, cache_sum = lax.map(one_sequence, (query_lat, query_rot, cache_latent, cache_rope, valid_len))
    tree_lat = latent_new.reshape(seq_count, prop_count, KVR)
    tree_rot = key_new.reshape(seq_count, prop_count, ROPE)
    tree_scores = jnp.einsum('sjhr,skr->sjhk', query_lat.astype(f32), tree_lat.astype(f32))
    tree_scores = (tree_scores + jnp.einsum('sjhp,skp->sjhk', query_rot.astype(f32), tree_rot.astype(f32))) * inv_root
    linked = (family > 0.5)[:, :, None, :]
    tree_peak = lax.optimization_barrier(jnp.max(jnp.where(linked, tree_scores, NEG_INF), axis=3))
    tree_weights = jnp.where(linked, jnp.exp(tree_scores - tree_peak[..., None]), 0.0)
    tree_mass = lax.optimization_barrier(jnp.sum(tree_weights, axis=3))
    tree_sum = jnp.einsum('sjhk,skr->sjhr', tree_weights.astype(bf16).astype(f32), tree_lat.astype(f32))
    top_all = jnp.maximum(cache_peak, tree_peak)
    scale_one = jnp.exp(cache_peak - top_all)
    scale_two = jnp.exp(tree_peak - top_all)
    mass_all = cache_mass * scale_one + tree_mass * scale_two
    sum_all = cache_sum * scale_one[..., None] + tree_sum * scale_two[..., None]
    attended = sum_all / mass_all[..., None]
    head_out = jnp.einsum('sjhr,rhv->sjhv', attended, w_up_value.astype(f32), precision=lax.Precision.HIGHEST)
    head_rows = head_out.astype(bf16).reshape(token_count, N_TP, HG * VD)
    group_weights = w_out.reshape(N_TP, HG * VD, model_dim)
    group_part = jnp.einsum('tgi,gio->gto', head_rows.astype(f32), group_weights.astype(f32))
    mixed_raw = lax.optimization_barrier(jnp.sum(group_part.astype(bf16).astype(f32), axis=0))
    mixed = normalize(mixed_raw, g_out).astype(bf16).reshape(seq_count, prop_count, model_dim)
    slot_index = jnp.arange(LEN, dtype=jnp.int32)[None, :] - valid_len[:, None]
    landed = (slot_index >= 0) & (slot_index < prop_count)
    clipped = jnp.clip(slot_index, 0, prop_count - 1).astype(jnp.int32)
    pick_lat = jnp.take_along_axis(tree_lat, jnp.broadcast_to(clipped[:, :, None], (seq_count, LEN, KVR)), axis=1)
    pick_rot = jnp.take_along_axis(tree_rot, jnp.broadcast_to(clipped[:, :, None], (seq_count, LEN, ROPE)), axis=1)
    new_latent = jnp.where(landed[:, :, None], pick_lat, cache_latent)
    new_rope = jnp.where(landed[:, :, None], pick_rot, cache_rope)
    return (mixed, new_latent, new_rope)
```

```python
import functools

import jax
import jax.numpy as jnp
from jax import lax
from jax.experimental import pallas as pl
from jax.experimental.pallas import tpu as pltpu
from jax.sharding import PartitionSpec as P

EPS = 1e-06
ROPE_BASE = 10000.0
NEG_INF = -1e30
LANES = 128
F32 = jnp.float32
BF16 = jnp.bfloat16
NT = (((1,), (1,)), ((), ()))


def dot(a, b):
    return jnp.dot(a, b, preferred_element_type=F32)


def dot_nt(a, b):
    return lax.dot_general(a, b, NT, preferred_element_type=F32)


def rotated(x, cosine, sine, rope):
    width = x.shape[1]
    lane = lax.broadcasted_iota(jnp.int32, x.shape, 1)
    front = lax.rem(lane, rope) < rope // 2
    partner = jnp.where(front, -pltpu.roll(x, width - rope // 2, 1), pltpu.roll(x, rope // 2, 1))
    return x * cosine + partner * sine


def column_to_row(column):
    rows = column.shape[0]
    wide = jnp.broadcast_to(column, (rows, LANES))
    if rows < LANES:
        wide = jnp.concatenate([wide, jnp.zeros((LANES - rows, LANES), F32)], axis=0)
    return wide.T[0:1, :]


def kernel(
    nk, nt, seqs, props, heads, qr, kvr, rope, vd, nope, model,
    valid_ref, tokens_ref, g_pre_ref, g_q_ref, g_out_ref, table_ref, mask_ref,
    wdq_hbm, wdkv_hbm, wkr_hbm, wuq_hbm, wqr_hbm, wuk_hbm, wuv_hbm, wout_hbm, lat_hbm, rot_hbm,
    mixed_ref, latnew_ref, keynew_ref,
    wdq, wdkv, wkr, wuq, wqr, wuk, wuv, wout, lat, rot,
    tok, buf1, buf2, buf3, lse3, buf4, buf5, qa, cs,
    load_sem, send1, recv1, send2, recv2, send3, recv3, send3b, recv3b, send4, recv4, send5, recv5,
):
    me_k = lax.axis_index("kv")
    me_t = lax.axis_index("tp")
    tokens = seqs * props
    group = tokens // nt
    rows = heads * tokens
    span = lat.shape[1]
    per_seq = heads * props

    barrier = pltpu.get_barrier_semaphore()
    for d in range(1, nk):
        pl.semaphore_signal(barrier, inc=1, device_id={"kv": lax.rem(me_k + d, nk)})
    for d in range(1, nt):
        pl.semaphore_signal(barrier, inc=1, device_id={"tp": lax.rem(me_t + d, nt)})

    loads = []
    for i, (src, dst) in enumerate(
        (
            (wdq_hbm, wdq), (wdkv_hbm, wdkv), (wkr_hbm, wkr), (wuq_hbm, wuq), (wqr_hbm, wqr),
            (wuk_hbm, wuk), (lat_hbm, lat), (rot_hbm, rot), (wuv_hbm, wuv), (wout_hbm, wout),
        )
    ):
        copy = pltpu.make_async_copy(src, dst, load_sem.at[i])
        copy.start()
        loads.append(copy)

    def exchange(buffer, axis, me, n, send, recv):
        copies = []
        for d in range(1, n):
            copy = pltpu.make_async_remote_copy(
                src_ref=buffer.at[me],
                dst_ref=buffer.at[me],
                send_sem=send.at[d - 1],
                recv_sem=recv.at[d - 1],
                device_id={axis: lax.rem(me + d, n)},
                device_id_type=pl.DeviceIdType.MESH,
            )
            copy.start()
            copies.append(copy)
        return copies

    sent = []

    tok[...] = tokens_ref[...].astype(F32)
    x = tok[pl.ds(pl.multiple_of(me_t * group, group), group), :]
    scaled = (x * g_pre_ref[...].astype(F32)).astype(BF16)
    squares = jnp.sum(x * x, axis=1, keepdims=True)
    for i in range(3):
        loads[i].wait()
    buf1[me_k, :, 0:qr] = dot(scaled, wdq[...])
    buf1[me_k, :, qr : qr + kvr] = dot(scaled, wdkv[...])
    buf1[me_k, :, qr + kvr : qr + kvr + LANES] = jnp.concatenate(
        [dot(scaled, wkr[...]), jnp.broadcast_to(squares, (group, LANES - rope))], axis=1
    )
    pl.semaphore_wait(barrier, nk - 1 + nt - 1)
    copies = exchange(buf1, "kv", me_k, nk, send1, recv1)
    sent += copies
    for copy in copies:
        copy.wait_recv()
    total = buf1[0]
    for k in range(1, nk):
        total = total + buf1[k]
    last = total[:, qr + kvr :]
    scale = lax.rsqrt(last[:, rope : rope + 1] / model + EPS)
    q_latent = total[:, 0:qr] * scale
    q_norm = (
        q_latent
        * lax.rsqrt(jnp.mean(q_latent * q_latent, axis=1, keepdims=True) + EPS)
        * g_q_ref[...].astype(F32)
    )
    kv_latent = total[:, qr : qr + kvr] * scale
    latent = kv_latent * lax.rsqrt(jnp.mean(kv_latent * kv_latent, axis=1, keepdims=True) + EPS)
    table = table_ref[pl.ds(pl.multiple_of(me_t * group, group), group), :]
    key = rotated(last * scale, table[:, 0:LANES], table[:, LANES:], rope)
    buf2[me_t, :, 0:qr] = q_norm.astype(BF16)
    buf2[me_t, :, qr : qr + kvr] = latent.astype(BF16)
    buf2[me_t, :, qr + kvr :] = key.astype(BF16)
    copies = exchange(buf2, "tp", me_t, nt, send2, recv2)
    sent += copies
    for i in range(3, 8):
        loads[i].wait()
    for copy in copies:
        copy.wait_recv()

    gathered = buf2[...].astype(F32).reshape(tokens, qr + kvr + LANES)
    q_all = gathered[:, 0:qr].astype(BF16)
    lat_new = gathered[:, qr : qr + kvr].astype(BF16)
    key_new = gathered[:, qr + kvr : qr + kvr + rope].astype(BF16)
    latnew_ref[...] = lat_new
    keynew_ref[...] = key_new

    q_nope = dot(q_all, wuq[...]).astype(BF16)
    q_raw = dot(q_all, wqr[...])
    copies_wide = heads * rope // LANES
    cosine = jnp.concatenate([table_ref[:, 0:LANES]] * copies_wide, axis=1)
    sine = jnp.concatenate([table_ref[:, LANES:]] * copies_wide, axis=1)
    q_rot = rotated(q_raw, cosine, sine, rope)
    lat_tiles = kvr // LANES
    for h in range(heads):
        part = dot_nt(
            q_nope[:, h * nope : (h + 1) * nope], wuk[:, h * nope : (h + 1) * nope]
        )
        for c in range(lat_tiles):
            qa[c, h * tokens : (h + 1) * tokens, :] = part[:, c * LANES : (c + 1) * LANES]
        qa[lat_tiles, h * tokens : (h + 1) * tokens, 0:rope] = q_rot[:, h * rope : (h + 1) * rope]

    inv_root = (nope + rope) ** (-0.5)
    offset = me_k * span
    column = lax.broadcasted_iota(jnp.int32, (per_seq, span), 1) + offset
    for s in range(seqs):
        pick = pl.ds(s, per_seq, stride=seqs)
        q_lat = jnp.concatenate([qa[c, pick, :] for c in range(lat_tiles)], axis=1).astype(BF16)
        q_pos = qa[lat_tiles, pick, :][:, 0:rope].astype(BF16)
        scores = (dot_nt(q_lat, lat[s]) + dot_nt(q_pos, rot[s])) * inv_root
        seen = column < valid_ref[s]
        peak = jnp.max(jnp.where(seen, scores, NEG_INF), axis=1, keepdims=True)
        weights = jnp.where(seen, jnp.exp(scores - peak), 0.0)
        mass = jnp.sum(weights, axis=1, keepdims=True)
        some = mass > 0.0
        safe = jnp.where(some, mass, 1.0)
        mean = dot(weights.astype(BF16), lat[s]) / safe
        lse = jnp.where(some, peak + jnp.log(safe), NEG_INF)
        for c in range(lat_tiles):
            cs[c, pick, :] = mean[:, c * LANES : (c + 1) * LANES]
        cs[lat_tiles, pick, :] = jnp.broadcast_to(lse, (per_seq, LANES))

    loads[8].wait()

    def up_value(means, h):
        high = means.astype(BF16)
        low = (means - high.astype(F32)).astype(BF16)
        weight = wuv[:, h * vd : (h + 1) * vd]
        return dot(high, weight) + dot(low, weight)

    for h in range(heads):
        rows_h = slice(h * tokens, (h + 1) * tokens)
        means = jnp.concatenate([cs[c, rows_h, :] for c in range(lat_tiles)], axis=1)
        buf3[me_k, rows_h, :] = up_value(means, h).astype(BF16)
    lse3[me_k] = cs[lat_tiles].T[0:1, :]
    copies = exchange(lse3, "kv", me_k, nk, send3b, recv3b)
    copies += exchange(buf3, "kv", me_k, nk, send3, recv3)
    sent += copies

    q_lat = jnp.concatenate([qa[c] for c in range(lat_tiles)], axis=1).astype(BF16)
    q_pos = qa[lat_tiles][:, 0:rope].astype(BF16)
    scores = (dot_nt(q_lat, lat_new) + dot_nt(q_pos, key_new)) * inv_root
    linked = jnp.concatenate([mask_ref[...]] * heads, axis=0) > 0.5
    peak = jnp.max(jnp.where(linked, scores, NEG_INF), axis=1, keepdims=True)
    weights = jnp.where(linked, jnp.exp(scores - peak), 0.0)
    mass = jnp.sum(weights, axis=1, keepdims=True)
    means = dot(weights.astype(BF16), lat_new) / mass
    tree_lse = peak + jnp.log(mass)
    tree_vals = jnp.concatenate(
        [up_value(means[h * tokens : (h + 1) * tokens], h) for h in range(heads)], axis=0
    )
    loads[9].wait()
    for copy in copies:
        copy.wait_recv()

    padding = jnp.full((LANES - nk, LANES), NEG_INF, F32)
    lses = jnp.concatenate([lse3[k] for k in range(nk)] + [padding], axis=0).T
    top = jnp.maximum(jnp.max(lses, axis=1, keepdims=True), tree_lse)
    share = jnp.exp(lses - top)
    tree_share = jnp.exp(tree_lse - top)
    divisor = jnp.sum(share, axis=1, keepdims=True) + tree_share
    merged = tree_share * tree_vals
    for k in range(nk):
        merged = merged + share[:, k : k + 1] * buf3[k].astype(F32)
    head_out = (merged / divisor).astype(BF16)
    head_rows = jnp.concatenate(
        [head_out[h * tokens : (h + 1) * tokens] for h in range(heads)], axis=1
    )
    buf4[me_t] = dot(head_rows, wout[...]).astype(BF16)
    copies = exchange(buf4, "tp", me_t, nt, send4, recv4)
    sent += copies
    for copy in copies:
        copy.wait_recv()
    mixed_raw = buf4[0].astype(F32)
    for t in range(1, nt):
        mixed_raw = mixed_raw + buf4[t].astype(F32)
    buf5[me_k] = column_to_row(jnp.sum(mixed_raw * mixed_raw, axis=1, keepdims=True))
    copies = exchange(buf5, "kv", me_k, nk, send5, recv5)
    sent += copies
    scaled_out = mixed_raw * g_out_ref[...].astype(F32)
    for copy in copies:
        copy.wait_recv()
    total_sq = buf5[0]
    for k in range(1, nk):
        total_sq = total_sq + buf5[k]
    factor = lax.rsqrt(total_sq / model + EPS)
    factor = jnp.broadcast_to(factor, (LANES, LANES)).T[0:tokens, 0:1]
    mixed_ref[...] = (scaled_out * factor).astype(BF16)
    for copy in sent:
        copy.wait_send()


def lineage(parents):
    props = parents.shape[1]
    index = jnp.arange(props, dtype=jnp.int32)
    rows = []
    for j in range(props):
        row = jnp.broadcast_to(index == j, (parents.shape[0], props))
        for m in range(j):
            row = row | ((parents[:, j : j + 1] == m) & rows[m])
        rows.append(row)
    return jnp.stack(rows, axis=1)


def local(
    nk,
    nt,
    tokens,
    prev_len,
    accepted,
    parents,
    cache_latent,
    cache_rope,
    g_pre,
    w_down_q,
    w_down_kv,
    w_key_rope,
    g_q,
    w_up_q,
    w_q_rope,
    w_up_key,
    w_up_value,
    w_out,
    g_out,
):
    seqs, props, width = tokens.shape
    count = seqs * props
    group = count // nt
    qr, heads, nope = w_up_q.shape
    rope = w_q_rope.shape[2]
    kvr = w_up_key.shape[0]
    vd = w_up_value.shape[2]
    span = cache_latent.shape[1]
    width_out = w_out.shape[1]
    rows = heads * count
    wide = qr + kvr + LANES

    valid_len = prev_len + accepted
    family = lineage(parents)
    depths = jnp.sum(family.astype(jnp.int32), axis=2) - 1
    positions = (valid_len[:, None] + depths).T.reshape(count)
    half = rope // 2
    frequency = ROPE_BASE ** (-jnp.arange(half, dtype=F32) / half)
    angles = positions.astype(F32)[:, None] * jnp.tile(frequency, LANES // half)
    table = jnp.concatenate([jnp.cos(angles), jnp.sin(angles)], axis=1)
    same = jnp.eye(seqs, dtype=F32)
    mask = (family.astype(F32).transpose(1, 0, 2)[:, :, :, None] * same[None, :, None, :]).reshape(
        count, count
    )
    rows_in = tokens.transpose(1, 0, 2).reshape(count, width)

    vmem = pl.BlockSpec(memory_space=pltpu.VMEM)
    anywhere = pl.BlockSpec(memory_space=pl.ANY)
    dma = pltpu.SemaphoreType.DMA
    weights = (
        w_down_q,
        w_down_kv,
        w_key_rope,
        w_up_q.reshape(qr, heads * nope),
        w_q_rope.reshape(qr, heads * rope),
        w_up_key.reshape(kvr, heads * nope),
        w_up_value.reshape(kvr, heads * vd),
        w_out,
        cache_latent,
        cache_rope,
    )
    mixed, lat_new, key_new = pl.pallas_call(
        functools.partial(
            kernel, nk, nt, seqs, props, heads, qr, kvr, rope, vd, nope, width * nk
        ),
        out_shape=(
            jax.ShapeDtypeStruct((count, width_out), BF16),
            jax.ShapeDtypeStruct((count, kvr), BF16),
            jax.ShapeDtypeStruct((count, rope), BF16),
        ),
        in_specs=[pl.BlockSpec(memory_space=pltpu.SMEM)] + [vmem] * 6 + [anywhere] * 10,
        out_specs=(vmem, vmem, vmem),
        scratch_shapes=[pltpu.VMEM(w.shape, BF16) for w in weights]
        + [
            pltpu.VMEM((count, width), F32),
            pltpu.VMEM((nk, group, wide), F32),
            pltpu.VMEM((nt, group, wide), BF16),
            pltpu.VMEM((nk, rows, vd), BF16),
            pltpu.VMEM((nk, 1, LANES), F32),
            pltpu.VMEM((nt, count, width_out), BF16),
            pltpu.VMEM((nk, 1, LANES), F32),
            pltpu.VMEM((kvr // LANES + 1, rows, LANES), F32),
            pltpu.VMEM((kvr // LANES + 1, rows, LANES), F32),
            dma((10,)),
            dma((nk - 1,)),
            dma((nk - 1,)),
            dma((nt - 1,)),
            dma((nt - 1,)),
            dma((nk - 1,)),
            dma((nk - 1,)),
            dma((nk - 1,)),
            dma((nk - 1,)),
            dma((nt - 1,)),
            dma((nt - 1,)),
            dma((nk - 1,)),
            dma((nk - 1,)),
        ],
        compiler_params=pltpu.CompilerParams(collective_id=0, has_side_effects=True),
    )(
        valid_len,
        rows_in,
        g_pre.reshape(1, width),
        g_q.reshape(1, qr),
        g_out.reshape(1, width_out),
        table,
        mask,
        *weights,
    )

    slot = (
        lax.axis_index("kv") * span
        + jnp.arange(span, dtype=jnp.int32)[None, :]
        - valid_len[:, None]
    )[:, :, None]
    new_latent = cache_latent
    new_rope = cache_rope
    for j in range(props):
        here = slot == j
        new_latent = jnp.where(here, lat_new[j * seqs : (j + 1) * seqs, None, :], new_latent)
        new_rope = jnp.where(here, key_new[j * seqs : (j + 1) * seqs, None, :], new_rope)
    return (
        mixed.reshape(props, seqs, width_out).transpose(1, 0, 2),
        new_latent,
        new_rope,
    )


def solution(mesh):
    return jax.shard_map(
        functools.partial(local, mesh.shape["kv"], mesh.shape["tp"]),
        mesh=mesh,
        in_specs=(
            P("grp", None, "kv"),
            P("grp"),
            P("grp"),
            P("grp", None),
            P("grp", "kv", None),
            P("grp", "kv", None),
            P("kv"),
            P("kv", None),
            P("kv", None),
            P("kv", None),
            P(),
            P(None, "tp", None),
            P(None, "tp", None),
            P(None, "tp", None),
            P(None, "tp", None),
            P("tp", "kv"),
            P("kv"),
        ),
        out_specs=(P("grp", None, "kv"), P("grp", "kv", None), P("grp", "kv", None)),
        check_vma=False,
    )
```

```python
import functools

import jax
import jax.numpy as jnp
import numpy as np
from jax import lax
from jax.experimental import pallas as pl
from jax.experimental.pallas import tpu as pltpu
from jax.sharding import PartitionSpec as P

EPS = 1e-06
ROPE_BASE = 10000.0
NEG_INF = -1e30
LANES = 128
F32 = jnp.float32
BF16 = jnp.bfloat16
NT = (((1,), (1,)), ((), ()))
TN = (((0,), (0,)), ((), ()))


def dot(a, b):
    return jnp.dot(a, b, preferred_element_type=F32)


def dot_nt(a, b):
    return lax.dot_general(a, b, NT, preferred_element_type=F32)


def rotated(x, cosine, sine, rope):
    width = x.shape[1]
    lane = lax.broadcasted_iota(jnp.int32, x.shape, 1)
    front = lax.rem(lane, rope) < rope // 2
    partner = jnp.where(front, -pltpu.roll(x, width - rope // 2, 1), pltpu.roll(x, rope // 2, 1))
    return x * cosine + partner * sine


def column_to_row(column):
    rows = column.shape[0]
    wide = jnp.broadcast_to(column, (rows, LANES))
    if rows < LANES:
        wide = jnp.concatenate([wide, jnp.zeros((LANES - rows, LANES), F32)], axis=0)
    return wide.T[0:1, :]


def kernel(
    nk, nt, seqs, props, heads, qr, kvr, rope, vd, nope, model,
    prev_ref, accepted_ref, parents_ref, tokens_ref, g_pre_ref, g_q_ref, g_out_ref,
    wdq_hbm, wdkv_hbm, wkr_hbm, wuq_hbm, wqr_hbm, wuk_hbm, wuv_hbm, wout_hbm, lat_hbm, rot_hbm,
    mixed_ref, latout_hbm, rotout_hbm,
    wdq, wdkv, wkr, wuq_raw, wqr, wuk_raw, wuv_raw, wout, lat, rot,
    wuq, wuk, wuv, spread, table_ref, lat_out, rot_out,
    tok, buf1, buf2, buf3, lse3, buf4, buf5, qa, cs,
    load_sem, store_sem, send1, recv1, send2, recv2, send3, recv3, send3b, recv3b, send4, recv4, send5, recv5,
):
    me_k = lax.axis_index("kv")
    me_t = lax.axis_index("tp")
    tokens = seqs * props
    group = tokens // nt
    rows = heads * tokens
    span = lat.shape[1]
    per_seq = heads * props

    barrier = pltpu.get_barrier_semaphore()
    for d in range(1, nk):
        pl.semaphore_signal(barrier, inc=1, device_id={"kv": lax.rem(me_k + d, nk)})
    for d in range(1, nt):
        pl.semaphore_signal(barrier, inc=1, device_id={"tp": lax.rem(me_t + d, nt)})

    loads = []
    for i, (src, dst) in enumerate(
        (
            (wdq_hbm, wdq), (wdkv_hbm, wdkv), (wkr_hbm, wkr), (wuq_hbm, wuq_raw), (wqr_hbm, wqr),
            (wuk_hbm, wuk_raw), (lat_hbm, lat), (rot_hbm, rot), (wuv_hbm, wuv_raw),
            (wout_hbm, wout),
        )
    ):
        copy = pltpu.make_async_copy(src, dst, load_sem.at[i])
        copy.start()
        loads.append(copy)

    def exchange(buffer, axis, me, n, send, recv):
        copies = []
        for d in range(1, n):
            copy = pltpu.make_async_remote_copy(
                src_ref=buffer.at[me],
                dst_ref=buffer.at[me],
                send_sem=send.at[d - 1],
                recv_sem=recv.at[d - 1],
                device_id={axis: lax.rem(me + d, n)},
                device_id_type=pl.DeviceIdType.MESH,
            )
            copy.start()
            copies.append(copy)
        return copies

    sent = []

    width = tokens_ref.shape[2]
    for s in range(seqs):
        own = tokens_ref[s].astype(F32)
        for c in range(tok.shape[0]):
            piece = own[:, c * LANES : min((c + 1) * LANES, width)]
            if piece.shape[1] < LANES:
                fill = jnp.zeros((props, LANES - piece.shape[1]), F32)
                piece = jnp.concatenate([piece, fill], axis=1)
            tok[c, pl.ds(s, props, stride=seqs), :] = piece
    mine = pl.ds(pl.multiple_of(me_t * group, group), group)
    x = jnp.concatenate([tok[c, mine, :] for c in range(tok.shape[0])], axis=1)[:, 0:width]
    scaled = (x * g_pre_ref[...].astype(F32).reshape(1, width)).astype(BF16)
    squares = jnp.sum(x * x, axis=1, keepdims=True)
    for i in range(3):
        loads[i].wait()
    buf1[me_k, :, 0:qr] = dot(scaled, wdq[...])
    buf1[me_k, :, qr : qr + kvr] = dot(scaled, wdkv[...])
    buf1[me_k, :, qr + kvr : qr + kvr + LANES] = jnp.concatenate(
        [dot_nt(scaled, wkr[...]), jnp.broadcast_to(squares, (group, LANES - rope))], axis=1
    )
    pl.semaphore_wait(barrier, nk - 1 + nt - 1)
    copies = exchange(buf1, "kv", me_k, nk, send1, recv1)
    sent += copies

    valid = [prev_ref[s] + accepted_ref[s] for s in range(seqs)]
    sublane = lax.broadcasted_iota(jnp.int32, (seqs, LANES), 0)
    lane = lax.broadcasted_iota(jnp.int32, (seqs, LANES), 1)
    place = [jnp.zeros((seqs, LANES), jnp.int32) for j in range(props)]
    kin = [jnp.zeros((seqs, LANES), jnp.int32) for j in range(props)]
    for s in range(seqs):
        depth, line = [], []
        for j in range(props):
            parent = parents_ref[j, s]
            deep, bits = jnp.int32(0), jnp.int32(1 << j)
            for m in range(j):
                deep = jnp.where(parent == m, depth[m] + 1, deep)
                bits = jnp.where(parent == m, line[m] + (1 << j), bits)
            depth.append(deep)
            line.append(bits)
            place[j] = jnp.where(sublane == s, valid[s] + deep, place[j])
            kin[j] = jnp.where(sublane == s, bits, kin[j])
    half = rope // 2
    frequency = jnp.zeros((1, LANES), F32)
    for i in range(half):
        value = float(np.float32(ROPE_BASE ** (-i / half)))
        frequency = jnp.where(lax.rem(lane[0:1], half) == i, value, frequency)
    angles = jnp.concatenate(place, axis=0).astype(F32) * frequency
    table_ref[:, 0:LANES] = jnp.cos(angles)
    table_ref[:, LANES:] = jnp.sin(angles)
    own_seq = lax.rem(lane, seqs) == sublane
    their = lax.div(lane, seqs)
    linked = jnp.concatenate(
        [
            (own_seq & ((lax.shift_right_logical(bits, their) & 1) == 1)).astype(F32)
            for bits in kin
        ],
        axis=0,
    )[:, 0:tokens]
    for i, raw, flat, size in (
        (3, wuq_raw, wuq, nope), (5, wuk_raw, wuk, nope), (8, wuv_raw, wuv, vd)
    ):
        loads[i].wait()
        count = raw.shape[0]
        depth_rows = count // heads
        spread[0:count, :] = raw[...].astype(F32)
        for h in range(heads):
            flat[:, h * size : (h + 1) * size] = spread[
                pl.ds(h, depth_rows, stride=heads), :
            ].astype(BF16)
    for i in (4, 6, 7):
        loads[i].wait()
    for copy in copies:
        copy.wait_recv()
    total = buf1[0]
    for k in range(1, nk):
        total = total + buf1[k]
    last = total[:, qr + kvr :]
    scale = lax.rsqrt(last[:, rope : rope + 1] / model + EPS)
    q_latent = total[:, 0:qr] * scale
    q_norm = (
        q_latent
        * lax.rsqrt(jnp.mean(q_latent * q_latent, axis=1, keepdims=True) + EPS)
        * g_q_ref[...].astype(F32).reshape(1, qr)
    )
    kv_latent = total[:, qr : qr + kvr] * scale
    latent = kv_latent * lax.rsqrt(jnp.mean(kv_latent * kv_latent, axis=1, keepdims=True) + EPS)
    table = table_ref[pl.ds(pl.multiple_of(me_t * group, group), group), :]
    key = rotated(last * scale, table[:, 0:LANES], table[:, LANES:], rope)
    buf2[me_t, :, 0:qr] = q_norm.astype(BF16)
    buf2[me_t, :, qr : qr + kvr] = latent.astype(BF16)
    buf2[me_t, :, qr + kvr :] = key.astype(BF16)
    copies = exchange(buf2, "tp", me_t, nt, send2, recv2)
    sent += copies
    for copy in copies:
        copy.wait_recv()

    gathered = buf2[...].astype(F32).reshape(tokens, qr + kvr + LANES)
    q_all = gathered[:, 0:qr].astype(BF16)
    lat_new = gathered[:, qr : qr + kvr].astype(BF16)
    key_new = gathered[:, qr + kvr : qr + kvr + rope].astype(BF16)

    q_nope = dot(q_all, wuq[...]).astype(BF16)
    q_raw = dot_nt(q_all, wqr[...])
    copies_wide = heads * rope // LANES
    cosine = jnp.concatenate([table_ref[:, 0:LANES]] * copies_wide, axis=1)
    sine = jnp.concatenate([table_ref[:, LANES:]] * copies_wide, axis=1)
    q_rot = rotated(q_raw, cosine, sine, rope)
    lat_tiles = kvr // LANES
    for h in range(heads):
        part = dot_nt(
            q_nope[:, h * nope : (h + 1) * nope], wuk[:, h * nope : (h + 1) * nope]
        )
        for c in range(lat_tiles):
            qa[c, h * tokens : (h + 1) * tokens, :] = part[:, c * LANES : (c + 1) * LANES]
        qa[lat_tiles, h * tokens : (h + 1) * tokens, 0:rope] = q_rot[:, h * rope : (h + 1) * rope]

    inv_root = (nope + rope) ** (-0.5)
    offset = me_k * span
    column = lax.broadcasted_iota(jnp.int32, (per_seq, span), 1) + offset
    for s in range(seqs):
        pick = pl.ds(s, per_seq, stride=seqs)
        q_lat = jnp.concatenate([qa[c, pick, :] for c in range(lat_tiles)], axis=1).astype(BF16)
        q_pos = qa[lat_tiles, pick, :][:, 0:rope].astype(BF16)
        scores = (dot_nt(q_lat, lat[s]) + dot(q_pos, rot[s])) * inv_root
        seen = column < valid[s]
        peak = jnp.max(jnp.where(seen, scores, NEG_INF), axis=1, keepdims=True)
        weights = jnp.where(seen, jnp.exp(scores - peak), 0.0)
        mass = jnp.sum(weights, axis=1, keepdims=True)
        some = mass > 0.0
        safe = jnp.where(some, mass, 1.0)
        mean = dot(weights.astype(BF16), lat[s]) / safe
        lse = jnp.where(some, peak + jnp.log(safe), NEG_INF)
        for c in range(lat_tiles):
            cs[c, pick, :] = mean[:, c * LANES : (c + 1) * LANES]
        cs[lat_tiles, pick, :] = jnp.broadcast_to(lse, (per_seq, LANES))

    def up_value(means, h):
        high = means.astype(BF16)
        low = (means - high.astype(F32)).astype(BF16)
        weight = wuv[:, h * vd : (h + 1) * vd]
        return dot(high, weight) + dot(low, weight)

    for h in range(heads):
        rows_h = slice(h * tokens, (h + 1) * tokens)
        means = jnp.concatenate([cs[c, rows_h, :] for c in range(lat_tiles)], axis=1)
        buf3[me_k, rows_h, :] = up_value(means, h).astype(BF16)
    lse3[me_k] = cs[lat_tiles].T[0:1, :]
    copies = exchange(lse3, "kv", me_k, nk, send3b, recv3b)
    copies += exchange(buf3, "kv", me_k, nk, send3, recv3)
    sent += copies

    q_lat = jnp.concatenate([qa[c] for c in range(lat_tiles)], axis=1).astype(BF16)
    q_pos = qa[lat_tiles][:, 0:rope].astype(BF16)
    scores = (dot_nt(q_lat, lat_new) + dot_nt(q_pos, key_new)) * inv_root
    linked = jnp.concatenate([linked] * heads, axis=0) > 0.5
    peak = jnp.max(jnp.where(linked, scores, NEG_INF), axis=1, keepdims=True)
    weights = jnp.where(linked, jnp.exp(scores - peak), 0.0)
    mass = jnp.sum(weights, axis=1, keepdims=True)
    means = dot(weights.astype(BF16), lat_new) / mass
    tree_lse = peak + jnp.log(mass)
    tree_vals = jnp.concatenate(
        [up_value(means[h * tokens : (h + 1) * tokens], h) for h in range(heads)], axis=0
    )
    row = lax.broadcasted_iota(jnp.int32, (tokens, span), 0)
    where_to = lax.broadcasted_iota(jnp.int32, (tokens, span), 1) + offset
    row_pos = lax.broadcasted_iota(jnp.int32, (span, kvr), 0) + offset
    lane_pos = lax.broadcasted_iota(jnp.int32, (rope, span), 1) + offset
    stores = []
    for s in range(seqs):
        hit = (where_to - lax.div(row, seqs) == valid[s]) & (lax.rem(row, seqs) == s)
        hit = hit.astype(F32).astype(BF16)
        put = lax.dot_general(hit, lat_new, TN, preferred_element_type=F32)
        landed = (row_pos >= valid[s]) & (row_pos < valid[s] + props)
        lat_out[s] = jnp.where(landed, put, lat[s].astype(F32)).astype(BF16)
        put = lax.dot_general(key_new, hit, TN, preferred_element_type=F32)
        landed = (lane_pos >= valid[s]) & (lane_pos < valid[s] + props)
        rot_out[s] = jnp.where(landed, put, rot[s].astype(F32)).astype(BF16)
    for i, (src, dst) in enumerate(((lat_out, latout_hbm), (rot_out, rotout_hbm))):
        copy = pltpu.make_async_copy(src, dst, store_sem.at[i])
        copy.start()
        stores.append(copy)
    loads[9].wait()
    for copy in copies:
        copy.wait_recv()

    padding = jnp.full((LANES - nk, LANES), NEG_INF, F32)
    lses = jnp.concatenate([lse3[k] for k in range(nk)] + [padding], axis=0).T
    top = jnp.maximum(jnp.max(lses, axis=1, keepdims=True), tree_lse)
    share = jnp.exp(lses - top)
    tree_share = jnp.exp(tree_lse - top)
    divisor = jnp.sum(share, axis=1, keepdims=True) + tree_share
    merged = tree_share * tree_vals
    for k in range(nk):
        merged = merged + share[:, k : k + 1] * buf3[k].astype(F32)
    head_out = (merged / divisor).astype(BF16)
    head_rows = jnp.concatenate(
        [head_out[h * tokens : (h + 1) * tokens] for h in range(heads)], axis=1
    )
    buf4[me_t] = dot(head_rows, wout[...]).astype(BF16)
    copies = exchange(buf4, "tp", me_t, nt, send4, recv4)
    sent += copies
    for copy in copies:
        copy.wait_recv()
    mixed_raw = buf4[0].astype(F32)
    for t in range(1, nt):
        mixed_raw = mixed_raw + buf4[t].astype(F32)
    buf5[me_k] = column_to_row(jnp.sum(mixed_raw * mixed_raw, axis=1, keepdims=True))
    copies = exchange(buf5, "kv", me_k, nk, send5, recv5)
    sent += copies
    scaled_out = mixed_raw * g_out_ref[...].astype(F32).reshape(1, mixed_raw.shape[1])
    for copy in copies:
        copy.wait_recv()
    total_sq = buf5[0]
    for k in range(1, nk):
        total_sq = total_sq + buf5[k]
    factor = lax.rsqrt(total_sq / model + EPS)
    factor = jnp.broadcast_to(factor, (LANES, LANES)).T[0:tokens, 0:1]
    mixed_ref[...] = (scaled_out * factor).astype(BF16)
    for copy in sent:
        copy.wait_send()
    for copy in stores:
        copy.wait()


def local(
    nk,
    nt,
    tokens,
    prev_len,
    accepted,
    parents,
    cache_latent,
    cache_rope,
    g_pre,
    w_down_q,
    w_down_kv,
    w_key_rope,
    g_q,
    w_up_q,
    w_q_rope,
    w_up_key,
    w_up_value,
    w_out,
    g_out,
):
    seqs, props, width = tokens.shape
    count = seqs * props
    group = count // nt
    qr, heads, nope = w_up_q.shape
    rope = w_q_rope.shape[2]
    kvr = w_up_key.shape[0]
    vd = w_up_value.shape[2]
    span = cache_latent.shape[1]
    width_out = w_out.shape[1]
    rows = heads * count
    wide = qr + kvr + LANES

    vmem = pl.BlockSpec(memory_space=pltpu.VMEM)
    anywhere = pl.BlockSpec(memory_space=pl.ANY)
    dma = pltpu.SemaphoreType.DMA
    weights = (
        w_down_q,
        w_down_kv,
        w_key_rope.T,
        w_up_q.reshape(qr * heads, nope),
        w_q_rope.transpose(1, 2, 0).reshape(heads * rope, qr),
        w_up_key.reshape(kvr * heads, nope),
        w_up_value.reshape(kvr * heads, vd),
        w_out,
        cache_latent,
        cache_rope.transpose(0, 2, 1),
    )
    mixed, new_latent, new_rope = pl.pallas_call(
        functools.partial(
            kernel, nk, nt, seqs, props, heads, qr, kvr, rope, vd, nope, width * nk
        ),
        out_shape=(
            jax.ShapeDtypeStruct((count, width_out), BF16),
            jax.ShapeDtypeStruct(cache_latent.shape, BF16),
            jax.ShapeDtypeStruct((seqs, rope, span), BF16),
        ),
        in_specs=[pl.BlockSpec(memory_space=pltpu.SMEM)] * 3 + [vmem] * 4 + [anywhere] * 10,
        out_specs=(vmem, anywhere, anywhere),
        scratch_shapes=[pltpu.VMEM(w.shape, BF16) for w in weights]
        + [
            pltpu.VMEM((qr, heads * nope), BF16),
            pltpu.VMEM((kvr, heads * nope), BF16),
            pltpu.VMEM((kvr, heads * vd), BF16),
            pltpu.VMEM((max(qr, kvr) * heads, LANES), F32),
            pltpu.VMEM((count, 2 * LANES), F32),
            pltpu.VMEM(cache_latent.shape, BF16),
            pltpu.VMEM((seqs, rope, span), BF16),
            pltpu.VMEM((pl.cdiv(width, LANES), count, LANES), F32),
            pltpu.VMEM((nk, group, wide), F32),
            pltpu.VMEM((nt, group, wide), BF16),
            pltpu.VMEM((nk, rows, vd), BF16),
            pltpu.VMEM((nk, 1, LANES), F32),
            pltpu.VMEM((nt, count, width_out), BF16),
            pltpu.VMEM((nk, 1, LANES), F32),
            pltpu.VMEM((kvr // LANES + 1, rows, LANES), F32),
            pltpu.VMEM((kvr // LANES + 1, rows, LANES), F32),
            dma((10,)),
            dma((2,)),
            dma((nk - 1,)),
            dma((nk - 1,)),
            dma((nt - 1,)),
            dma((nt - 1,)),
            dma((nk - 1,)),
            dma((nk - 1,)),
            dma((nk - 1,)),
            dma((nk - 1,)),
            dma((nt - 1,)),
            dma((nt - 1,)),
            dma((nk - 1,)),
            dma((nk - 1,)),
        ],
        compiler_params=pltpu.CompilerParams(collective_id=0, has_side_effects=True),
    )(
        prev_len,
        accepted,
        parents.T,
        tokens,
        g_pre,
        g_q,
        g_out,
        *weights,
    )

    return (
        mixed.reshape(props, seqs, width_out).transpose(1, 0, 2),
        new_latent,
        new_rope.transpose(0, 2, 1),
    )


def solution(mesh):
    return jax.shard_map(
        functools.partial(local, mesh.shape["kv"], mesh.shape["tp"]),
        mesh=mesh,
        in_specs=(
            P("grp", None, "kv"),
            P("grp"),
            P("grp"),
            P("grp", None),
            P("grp", "kv", None),
            P("grp", "kv", None),
            P("kv"),
            P("kv", None),
            P("kv", None),
            P("kv", None),
            P(),
            P(None, "tp", None),
            P(None, "tp", None),
            P(None, "tp", None),
            P(None, "tp", None),
            P("tp", "kv"),
            P("kv"),
        ),
        out_specs=(P("grp", None, "kv"), P("grp", "kv", None), P("grp", "kv", None)),
        check_vma=False,
    )
```
